32 devices in a mesh: fs: 16 (over z, y, x), tp: 2 (over core).
Axes of the slice: x: 2, y: 2, z: 4, core: 2. Of those that a mesh axis runs over, the one named last changes fastest.
Arguments:
- tokens: bfloat16 [6144, 2048], P('fs', 'tp'), may hold values from -6 to 6
- outer_gate: bfloat16 [2048, 2048], P('fs', 'tp'), may hold values from -0.125 to 0.125
- inner_gate: bfloat16 [2048, 2048], P('fs', 'tp'), may hold values from -0.125 to 0.125
- mix_value: bfloat16 [2048, 2048], P('fs', 'tp'), may hold values from -0.125 to 0.125
- mix_taps: bfloat16 [3, 2048], P(None, 'tp'), may hold values from -3 to 3
- mix_out: bfloat16 [2048, 2048], P('tp', 'fs'), may hold values from -0.1875 to 0.1875
- mix_gain: bfloat16 [2048], P('tp'), may hold values from 0.099609375 to 1.8984375
- ffn_gate: bfloat16 [2048, 3072], P('fs', 'tp'), may hold values from -0.125 to 0.125
- ffn_value: bfloat16 [2048, 3072], P('fs', 'tp'), may hold values from -0.125 to 0.125
- gate_taps: bfloat16 [3, 3072], P(None, 'tp'), may hold values from -3 to 3
- value_taps: bfloat16 [3, 3072], P(None, 'tp'), may hold values from -3 to 3
- ffn_down: bfloat16 [3072, 2048], P('tp', 'fs'), may hold values from -0.15625 to 0.15625
- ffn_gain: bfloat16 [2048], P('tp'), may hold values from 0.099609375 to 1.8984375
Outputs:
- layer_out: bfloat16 [6144, 2048], P('fs', 'tp')
The draws below stay inside these ranges and needn't reach their ends.
All inputs are finite; a program needn't handle non-finite values.
Results may differ from the reference program's by a relative error of at most 0.015.
Values may be sent and summed in bfloat16 or wider, within the bound.
No kernel may reach another device: no remote copies, remote signals or barrier semaphores. Data moves between devices by JAX's collectives and lax.ppermute only.
A program may use at most 64 MiB of HBM per device.

```python
import jax
import jax.numpy as jnp
from jax import lax

D = 2048
F = 3072
SEQ_LEN = 128
TOKENS = 6144
N_TP = 2


def with_spikes(values, own_key, source, target, blocks, factor):
    def block_of(dim):
        return (jnp.arange(values.shape[dim]) // (values.shape[dim] // blocks)).reshape((-1,) + (1,) * (values.ndim - 1 - dim))

    one_side = jax.random.permutation(own_key, blocks)[block_of(target)]
    far = (block_of(target) + blocks // 2) % blocks
    return jnp.where((block_of(source) == one_side) | (block_of(source) == far), factor * values, values)


def shard_levels(key, shape, pieces, smallest, high):
    loudness = 1.0
    for axis_at, shards_of in pieces:
        heights = jax.random.uniform(jax.random.fold_in(jax.random.fold_in(key, 6), axis_at), (shards_of,), jnp.float32, smallest / len(pieces), high / len(pieces))
        loudness = loudness * jnp.repeat(jnp.exp(heights), shape[axis_at] // shards_of).reshape((-1,) + (1,) * (len(shape) - 1 - axis_at))
    return loudness


def noise(stream_key, extent, scale, most, pieces=(), kind=jnp.bfloat16):
    values = jax.random.normal(stream_key, extent, jnp.float32) * scale
    if len(pieces) > 0:
        values = shard_levels(stream_key, extent, pieces, -0.22, 0.18) * values
    return jnp.clip(values, min=-most, max=most).astype(kind)


def heavy_noise(stream_key, extent, deviation, bound, cuts, heavy, kind=jnp.bfloat16):
    drawn = deviation * jax.random.normal(stream_key, extent, jnp.float32)
    if cuts:
        drawn = drawn * shard_levels(stream_key, extent, cuts, -0.22, 0.18)
    return jnp.clip(with_spikes(drawn, jax.random.fold_in(stream_key, 3), *heavy), -bound, bound).astype(kind)


def setup_inputs(seed: int = 0) -> dict:
    streams_of = jax.random.split(jax.random.key(seed), 14)
    return {
        "tokens": noise(streams_of[0], (TOKENS, D), 1.0, 6.0, ((0, 16), (1, 2))),
        "outer_gate": noise(streams_of[1], (D, D), D ** -0.5, 0.125, ((0, 16), (1, 2))),
        "inner_gate": noise(streams_of[2], (D, D), D ** -0.5, 0.125, ((0, 16), (1, 2))),
        "mix_value": noise(streams_of[3], (D, D), D ** -0.5, 0.125, ((0, 16), (1, 2))),
        "mix_taps": noise(streams_of[4], (3, D), 0.577, 3.0, ((1, 2),)),
        "mix_out": heavy_noise(streams_of[5], (D, D), D ** -0.5, 0.1875, ((0, 2), (1, 16)), (0, 1, 16, 2.0)),
        "mix_gain": jnp.clip(1.0 + 0.18 * jax.random.normal(streams_of[6], (D,), jnp.float32), 0.099609375, 1.8984375).astype(jnp.bfloat16),
        "ffn_gate": noise(streams_of[7], (D, F), D ** -0.5, 0.125, ((0, 16), (1, 2))),
        "ffn_value": noise(streams_of[8], (D, F), D ** -0.5, 0.125, ((0, 16), (1, 2))),
        "gate_taps": noise(streams_of[9], (3, F), 0.577, 3.0, ((1, 2),)),
        "value_taps": noise(streams_of[10], (3, F), 0.577, 3.0, ((1, 2),)),
        "ffn_down": heavy_noise(streams_of[11], (F, D), F ** -0.5, 0.15625, ((0, 2), (1, 16)), (0, 1, 16, 2.0)),
        "ffn_gain": jnp.clip(1.0 + 0.18 * jax.random.normal(streams_of[12], (D,), jnp.float32), 0.099609375, 1.8984375).astype(jnp.bfloat16),
    }


residual_scale = 8.0 ** 0.25
norm_epsilon = 1e-05

def stored(values):
    return lax.optimization_barrier(values.astype(jnp.bfloat16)).astype(jnp.float32)

def shift_rows(values, offset):
    position = jnp.arange(values.shape[0]) % SEQ_LEN
    shifted = jnp.concatenate([jnp.zeros((offset, values.shape[1]), values.dtype), values[:-offset]], axis=0)
    return jnp.where((position >= offset)[:, None], shifted, jnp.zeros_like(shifted))

def causal_taps(values, taps):
    weights = taps.astype(jnp.float32)
    return values * weights[2] + shift_rows(values, 1) * weights[1] + shift_rows(values, 2) * weights[0]

def norm_rows(hidden, gain):
    mean = lax.optimization_barrier(jnp.mean(hidden, axis=1, keepdims=True))
    spread = lax.optimization_barrier(jnp.mean(jnp.square(hidden - mean), axis=1, keepdims=True))
    return ((hidden - mean) * lax.rsqrt(spread + norm_epsilon) * gain.astype(jnp.float32)).astype(jnp.bfloat16)

def split_sum(left, right):
    width = left.shape[1] // N_TP
    total = jnp.zeros((left.shape[0], right.shape[1]), jnp.float32)
    for index in range(N_TP):
        term = jnp.dot(left[:, index * width:(index + 1) * width], right[index * width:(index + 1) * width], preferred_element_type=jnp.float32)
        total = total + stored(term)
    return total

def reference(tokens, outer_gate, inner_gate, mix_value, mix_taps, mix_out, mix_gain, ffn_gate, ffn_value, gate_taps, value_taps, ffn_down, ffn_gain):
    outer = stored(jnp.dot(tokens, outer_gate, preferred_element_type=jnp.float32))
    inner = stored(jnp.dot(tokens, inner_gate, preferred_element_type=jnp.float32))
    values = stored(jnp.dot(tokens, mix_value, preferred_element_type=jnp.float32))
    gated = (outer * causal_taps(inner * values, mix_taps)).astype(jnp.bfloat16)
    mixer_branch = split_sum(gated, mix_out)
    first = norm_rows(residual_scale * tokens.astype(jnp.float32) + mixer_branch, mix_gain)
    gate_up = stored(jnp.dot(first, ffn_gate, preferred_element_type=jnp.float32))
    value_up = stored(jnp.dot(first, ffn_value, preferred_element_type=jnp.float32))
    hidden = (jax.nn.silu(causal_taps(gate_up, gate_taps)) * causal_taps(value_up, value_taps)).astype(jnp.bfloat16)
    ffn_branch = split_sum(hidden, ffn_down)
    return norm_rows(residual_scale * first.astype(jnp.float32) + ffn_branch, ffn_gain)
```

```python
import jax
import jax.numpy as jnp
from jax import lax
from jax.sharding import PartitionSpec as P

SEQ_LEN = 128


residual_scale = 8.0**0.25
norm_epsilon = 1e-05

PLANE = 4
LINE = 4


def stored(values):
    return lax.optimization_barrier(values.astype(jnp.bfloat16)).astype(jnp.float32)


def shift_rows(values, offset):
    position = jnp.arange(values.shape[0]) % SEQ_LEN
    shifted = jnp.concatenate(
        [jnp.zeros((offset, values.shape[1]), values.dtype), values[:-offset]], axis=0
    )
    return jnp.where((position >= offset)[:, None], shifted, jnp.zeros_like(shifted))


def causal_taps(values, taps):
    weights = taps.astype(jnp.float32)
    return (
        values * weights[2]
        + shift_rows(values, 1) * weights[1]
        + shift_rows(values, 2) * weights[0]
    )


def fold_rows(whole, pieces):
    return tuple((jnp.dot(whole, piece, preferred_element_type=jnp.float32) for piece in pieces))


def norm_shares(prenorm, gain):
    width = prenorm.shape[1] * lax.axis_size("tp")
    row_sums = jnp.sum(prenorm, axis=1)
    row_squares = jnp.sum(prenorm * prenorm, axis=1)
    total, total_squares = lax.psum((row_sums, row_squares), "tp")
    mean = total / width
    spread = total_squares / width - mean * mean
    scaled = (prenorm - mean[:, None]) * lax.rsqrt(spread[:, None] + norm_epsilon)
    return (scaled * gain.astype(jnp.float32)).astype(jnp.bfloat16)


def gathered_body(
    tokens,
    outer_gate,
    inner_gate,
    mix_value,
    mix_taps,
    mix_out,
    mix_gain,
    ffn_gate,
    ffn_value,
    gate_taps,
    value_taps,
    ffn_down,
    ffn_gain,
):
    whole_tokens = lax.all_gather(tokens, "tp", axis=1, tiled=True)
    outer, inner, values = fold_rows(
        whole_tokens,
        (
            lax.all_gather(outer_gate, "fs", axis=0, tiled=True),
            lax.all_gather(inner_gate, "fs", axis=0, tiled=True),
            lax.all_gather(mix_value, "fs", axis=0, tiled=True),
        ),
    )
    outer, inner, values = (stored(outer), stored(inner), stored(values))
    gated = (outer * causal_taps(inner * values, mix_taps)).astype(jnp.bfloat16)
    mixer_terms = jnp.dot(
        gated, lax.all_gather(mix_out, "fs", axis=1, tiled=True), preferred_element_type=jnp.float32
    )
    mixer_branch = lax.psum_scatter(
        mixer_terms.astype(jnp.bfloat16), "tp", scatter_dimension=1, tiled=True
    ).astype(jnp.float32)
    first_own = norm_shares(residual_scale * tokens.astype(jnp.float32) + mixer_branch, mix_gain)
    first_whole = lax.all_gather(first_own, "tp", axis=1, tiled=True)
    gate_up, value_up = fold_rows(
        first_whole,
        (
            lax.all_gather(ffn_gate, "fs", axis=0, tiled=True),
            lax.all_gather(ffn_value, "fs", axis=0, tiled=True),
        ),
    )
    gate_up, value_up = (stored(gate_up), stored(value_up))
    hidden = (
        jax.nn.silu(causal_taps(gate_up, gate_taps)) * causal_taps(value_up, value_taps)
    ).astype(jnp.bfloat16)
    ffn_terms = jnp.dot(
        hidden,
        lax.all_gather(ffn_down, "fs", axis=1, tiled=True),
        preferred_element_type=jnp.float32,
    )
    ffn_branch = lax.psum_scatter(
        ffn_terms.astype(jnp.bfloat16), "tp", scatter_dimension=1, tiled=True
    ).astype(jnp.float32)
    return norm_shares(residual_scale * first_own.astype(jnp.float32) + ffn_branch, ffn_gain)


def planes_body(
    tokens,
    outer_gate,
    inner_gate,
    mix_value,
    mix_taps,
    mix_out,
    mix_gain,
    ffn_gate,
    ffn_value,
    gate_taps,
    value_taps,
    ffn_down,
    ffn_gain,
):
    place = lax.axis_index("fs")
    core = lax.axis_index("tp")
    spot, level = place % PLANE, place // PLANE
    everyone = range(PLANE * LINE)

    def swap(piece, other):
        return lax.ppermute(piece, "fs", [(at, at ^ other) for at in everyone])

    def cross(piece):
        return lax.ppermute(piece, "tp", [(0, 1), (1, 0)])

    def lift(piece, moves):
        pairs = [(a * PLANE + k, b * PLANE + k) for a, b in moves for k in range(PLANE)]
        return lax.ppermute(piece, "fs", pairs)

    def quarter(array, axis, index):
        width = array.shape[axis] // PLANE
        return lax.dynamic_slice_in_dim(array, index * width, width, axis)

    def spread_plane(arrays, axis):
        pieces = []
        for other in range(PLANE):
            cut = [quarter(array, axis, spot ^ other) for array in arrays]
            piece = jnp.concatenate(cut, axis=1)
            pieces.append(swap(piece, other) if other else piece)
        odd, far = spot % 2 == 1, spot >= 2
        pick = jnp.where
        pieces = [
            pick(odd, pieces[1], pieces[0]),
            pick(odd, pieces[0], pieces[1]),
            pick(odd, pieces[3], pieces[2]),
            pick(odd, pieces[2], pieces[3]),
        ]
        pieces = [pick(far, pieces[k ^ 2], pieces[k]) for k in range(PLANE)]
        return jnp.concatenate(pieces, axis=1 - axis)

    def gather_line(own):
        pair = lift(own, [(0, 1), (1, 0), (2, 3), (3, 2)])
        near = lift(own, [(1, 2), (2, 1)])
        far = lift(pair, [(1, 2), (2, 1)])
        near_out = lift(near, [(1, 0), (2, 3)])
        far_out = lift(far, [(1, 0), (2, 3)])
        middle = (level == 1) | (level == 2)
        near = jnp.where(middle, near, near_out)
        far = jnp.where(middle, far, far_out)
        even = level % 2 == 0

        def half(which):
            mine = level // 2 == which
            low = jnp.where(mine, jnp.where(even, own, pair), jnp.where(which == 0, far, near))
            high = jnp.where(mine, jnp.where(even, pair, own), jnp.where(which == 0, near, far))
            return low, high

        return half(core), half(1 - core)

    def reduce_plane(rows, own_columns, other_columns):
        own = None
        arrived = []
        for k in (3, 1, 2, 0):
            away = jnp.dot(rows[k], other_columns, preferred_element_type=jnp.float32)
            here = jnp.dot(rows[k], own_columns, preferred_element_type=jnp.float32)
            both = here + cross(away.astype(jnp.bfloat16)).astype(jnp.float32)
            if k:
                arrived.append(swap(both.astype(jnp.bfloat16), k).astype(jnp.float32))
            else:
                own = both
        return own + (arrived[0] + arrived[1] + arrived[2])

    into = spread_plane((outer_gate, inner_gate, mix_value), 1)
    own_into, other_into = gather_line(into)
    token_blocks = [tokens if k == 0 else swap(tokens, k) for k in range(PLANE)]
    whole = jnp.concatenate(
        [jnp.concatenate([block, cross(block)], axis=1) for block in token_blocks], axis=0
    )
    own_out, other_out = gather_line(spread_plane((mix_out,), 0))
    own_up, other_up = gather_line(spread_plane((ffn_gate, ffn_value), 1))
    own_down, other_down = gather_line(spread_plane((ffn_down,), 0))

    into = jnp.concatenate([*own_into, *other_into], axis=0)
    projected = jnp.dot(whole, into, preferred_element_type=jnp.float32)
    outer, inner, values = (
        stored(part) for part in jnp.split(projected, 3, axis=1)
    )
    gated = (outer * causal_taps(inner * values, quarter(mix_taps, 1, spot))).astype(jnp.bfloat16)
    mixer_branch = reduce_plane(
        jnp.split(gated, PLANE, axis=0),
        jnp.concatenate(own_out, axis=1),
        jnp.concatenate(other_out, axis=1),
    )
    first_own = norm_shares(residual_scale * tokens.astype(jnp.float32) + mixer_branch, mix_gain)

    up = jnp.concatenate([*own_up, *other_up], axis=0)
    gate_share, value_share = quarter(gate_taps, 1, spot), quarter(value_taps, 1, spot)
    hidden = [None] * PLANE
    for k in (0, 3, 1, 2):
        block = swap(first_own, k) if k else first_own
        block = jnp.concatenate([block, cross(block)], axis=1)
        raised = jnp.dot(block, up, preferred_element_type=jnp.float32)
        gate_up, value_up = (stored(part) for part in jnp.split(raised, 2, axis=1))
        hidden[k] = (
            jax.nn.silu(causal_taps(gate_up, gate_share)) * causal_taps(value_up, value_share)
        ).astype(jnp.bfloat16)
    ffn_branch = reduce_plane(
        hidden, jnp.concatenate(own_down, axis=1), jnp.concatenate(other_down, axis=1)
    )
    return norm_shares(residual_scale * first_own.astype(jnp.float32) + ffn_branch, ffn_gain)


def solution(mesh):
    placed = (
        P("fs", "tp"),
        P("fs", "tp"),
        P("fs", "tp"),
        P("fs", "tp"),
        P(None, "tp"),
        P("tp", "fs"),
        P("tp"),
        P("fs", "tp"),
        P("fs", "tp"),
        P(None, "tp"),
        P(None, "tp"),
        P("tp", "fs"),
        P("tp"),
    )
    planes = mesh.shape["fs"] == PLANE * LINE and mesh.shape["tp"] == 2
    body = planes_body if planes else gathered_body
    return jax.shard_map(body, mesh=mesh, in_specs=placed, out_specs=P("fs", "tp"), check_vma=False)
```
